32 devices in a mesh: sp: 16 (over z, y, x), tp: 2 (over core).
Axes of the slice: x: 2, y: 2, z: 4, core: 2. Of those that a mesh axis runs over, the one named last changes fastest.
Arguments:
- out_grad: bfloat16 [3584, 2048], P('sp'), may hold values from -6 to 6
- moe_input: bfloat16 [3584, 2048], P('sp'), may hold values from -6 to 6
- routes: int32 [3584, 2], P('sp'), may hold values from 0 to 15, all different within a row; in each aligned block of 224 rows (0 to 223, 224 to 447, ...) at most 56 rows name the same one
- route_weights: float32 [3584, 2], P('sp'), may hold values from 0.2 to 1
- conv_result: bfloat16 [3584, 1024], P('sp', 'tp'), may hold values from -60 to 60
- glu_value: bfloat16 [3584, 1024], P('sp', 'tp'), may hold values from -6 to 6
- glu_gate: bfloat16 [3584, 1024], P('sp', 'tp'), may hold values from -6 to 6
- conv_taps: bfloat16 [31, 1024], P(None, 'tp'), may hold values from -1 to 1
- norm_gain: float32 [1024], P('tp'), may hold values from 0.1 to 1.9
- proj_weight: bfloat16 [2048, 1024], P(None, 'tp'), may hold values from -0.1875 to 0.1875
- expert_gate: bfloat16 [16, 2048, 1024], P('sp', None, 'tp'), may hold values from -0.125 to 0.125
- expert_up: bfloat16 [16, 2048, 1024], P('sp', None, 'tp'), may hold values from -0.125 to 0.125
- expert_down: bfloat16 [16, 1024, 2048], P('sp', 'tp'), may hold values from -0.1875 to 0.1875
Outputs:
- input_grad: bfloat16 [3584, 2048], P('sp')
- proj_grad: float32 [2048, 1024], P('sp', 'tp')
- gate_grad: float32 [16, 2048, 1024], P('sp', None, 'tp')
- up_grad: float32 [16, 2048, 1024], P('sp', None, 'tp')
- down_grad: float32 [16, 1024, 2048], P('sp', 'tp')
- value_grad: bfloat16 [3584, 1024], P('sp', 'tp')
- gate_side_grad: bfloat16 [3584, 1024], P('sp', 'tp')
The draws below stay inside these ranges and needn't reach their ends.
Inputs may be any that keep to these rules, and one draw needn't show every extreme that they name: `routes`: in each aligned block of 224 tokens no expert is named more than 56 times, a bound that some block reaches; a token's experts differ.
All inputs are finite; a program needn't handle non-finite values.
Results may differ from the reference program's by a relative error of at most 0.0061.
Values may be sent and summed in bfloat16 or wider, within the bound.
A program may use at most 128 MiB of HBM per device.

```python
import math
import jax
import jax.numpy as jnp
import numpy as np
from jax import lax

D = 2048
CH = 1024
FFE = 1024
CONV_K = 31
TOP = 2
TOK_DEV = 224
TOKENS = 3584
EXPERTS = 16
CAP = 56
N_SP = 16
N_TP = 2


def draw_conv_result(key, part):
    first_key = jax.random.fold_in(jax.random.fold_in(key, 17), 0)
    channel = jnp.arange(CH, dtype=jnp.float32) / CH
    scale = (10.0 ** channel)[None, :]
    values = jnp.clip(jax.random.normal(first_key, (TOKENS, CH), jnp.float32), -6.0, 6.0) * scale
    return values.astype(jnp.bfloat16)


def with_spikes(entries, stream_key, source, target, blocks, factor):
    owner, partner = [(jnp.arange(entries.shape[dim]) // (entries.shape[dim] // blocks)).reshape([-1 if axis == dim else 1 for axis in range(entries.ndim)]) for dim in (source, target)]
    chosen = jax.random.permutation(stream_key, blocks)[partner]
    strong = (owner == chosen) | (owner == (partner + blocks // 2) % blocks)
    return jnp.where(strong, factor * entries, entries)


def steps_of(stream_key, extent, cuts, smallest, high):
    level = 1.0
    for axis_at, shards_of in cuts:
        heights = jax.random.uniform(jax.random.fold_in(jax.random.fold_in(stream_key, 6), axis_at), (shards_of,), jnp.float32, smallest / len(cuts), high / len(cuts))
        level = level * jnp.repeat(jnp.exp(heights), extent[axis_at] // shards_of).reshape((-1,) + (1,) * (len(extent) - 1 - axis_at))
    return level


def deal_out(key, own, number, rows, number_of, top, bound, skew):
    order = jax.random.permutation(key, number_of)
    heavy_load, common = load_shares(number_of, rows * top, bound, skew, True), load_shares(number_of, rows * top, bound, skew, False)
    places = jnp.arange(number_of)

    def named(tallies, offset_by):
        used = int((tallies > 0).sum())
        fixed = max(1, used // 4)
        moved = fixed + (places - fixed + offset_by * (used - fixed)) % max(1, number_of - fixed)
        return jnp.zeros((number_of,), jnp.int32).at[order[jnp.where(places < fixed, places, moved)]].set(jnp.asarray(tallies, jnp.int32))

    tallies = jnp.where(number % 4 == 0, named(heavy_load, number // 4), named(common, number - number // 4 - 1))
    mixed = jax.random.permutation(jax.random.fold_in(own, 3), number_of)
    donor, taker = mixed[0:number_of // 2 * 2:2], mixed[1:number_of // 2 * 2:2]
    margin = jnp.minimum(tallies[donor] - 1, bound - tallies[taker]) // 2
    margin = jnp.where((donor == order[0]) | (taker == order[0]) | (tallies[taker] == 0), 0, jnp.maximum(margin, 0))
    moved = jax.random.randint(jax.random.fold_in(own, 4), (number_of // 2,), 0, 1 << 20) % (margin + 1)
    tallies = tallies.at[donor].add(-moved).at[taker].add(moved)
    members = jnp.searchsorted(jnp.cumsum(tallies), jnp.arange(rows * top), side="right").astype(jnp.int32)
    grid = members.reshape(top, rows).T
    grid = grid[jax.random.permutation(jax.random.fold_in(own, 1), rows)]
    offset_by = jax.random.randint(jax.random.fold_in(own, 2), (rows, 1), 0, top)
    return jnp.take_along_axis(grid, (jnp.arange(top)[None, :] + offset_by) % top, axis=1)


def load_shares(number_of, total, most, slope, full):
    loads = [(1 << 20) // math.isqrt(rank ** slope) + 1 for rank in range(1, number_of + 1)]
    largest = most if full else min(most, max(-(-total // number_of), total * loads[0] // sum(loads)))
    least = 1 if total - largest >= number_of - 1 else 0
    holding, rest = [largest] + [least] * (number_of - 1), total - largest - least * (number_of - 1)
    while rest > 0:
        movable = [i for i in range(1, number_of) if holding[i] < largest] or [i for i in range(1, number_of) if holding[i] < most]
        whole, left = sum([loads[i] for i in movable]), rest
        for i in movable:
            extra = min(most - holding[i], max(1, left * loads[i] // whole), rest)
            holding[i] = holding[i] + extra
            rest = rest - extra
    return np.array(holding)


def centred(key, dims, deviation, limit, pieces=(), kind=jnp.bfloat16):
    drawn = jax.random.normal(key, dims, jnp.float32) * deviation
    if len(pieces) > 0:
        drawn = steps_of(key, dims, pieces, -0.22, 0.18) * drawn
    return jnp.clip(drawn, min=-limit, max=limit).astype(kind)


def gaussian_with(stream_key, extent, width, bound, pieces, heavy, kind=jnp.bfloat16):
    entries = width * jax.random.normal(stream_key, extent, jnp.float32)
    if pieces:
        entries = entries * steps_of(stream_key, extent, pieces, -0.22, 0.18)
    return jnp.clip(with_spikes(entries, jax.random.fold_in(stream_key, 3), *heavy), -bound, bound).astype(kind)


def setup_inputs(seed: int = 0) -> dict:
    seeds = jax.random.split(jax.random.key(seed), 14)
    out_grad = gaussian_with(seeds[0], (TOKENS, D), 1.0, 6.0, ((0, 16),), (0, 1, 16, 2.0))
    moe_input = centred(seeds[1], (TOKENS, D), 1.0, 6.0, ((0, 16),))
    routes_keys = jax.random.split(jax.random.fold_in(seeds[2], 1), TOKENS // TOK_DEV)
    routes_turns = jax.random.permutation(jax.random.fold_in(seeds[2], 3), TOKENS // TOK_DEV)
    routes = jax.vmap(lambda own, number: deal_out(jax.random.fold_in(seeds[2], 2), own, number, TOK_DEV, EXPERTS, TOP, CAP, 1))(routes_keys, routes_turns).reshape((TOKENS, TOP))
    route_weights = jnp.clip(0.2 + 0.8 * jax.random.uniform(seeds[3], (TOKENS, TOP), jnp.float32) ** steps_of(seeds[3], (TOKENS, TOP), ((0, 16),), -0.2, 0.2), 0.2, 1.0)
    conv_result = draw_conv_result(jax.random.fold_in(seeds[13], 71), 0)
    glu_value = centred(seeds[5], (TOKENS, CH), 1.0, 6.0, ((0, 16), (1, 2)))
    glu_gate = centred(seeds[6], (TOKENS, CH), 1.0, 6.0, ((0, 16), (1, 2)))
    conv_taps = centred(seeds[7], (CONV_K, CH), CONV_K ** -0.5, 1.0, ((1, 2),))
    norm_gain = jnp.clip(1.0 + 0.18 * jax.random.normal(seeds[8], (CH,), jnp.float32), 0.1, 1.9)
    proj_weight = centred(seeds[9], (D, CH), CH ** -0.5, 0.1875, ((1, 2),))
    expert_gate = centred(seeds[10], (EXPERTS, D, FFE), D ** -0.5, 0.125, ((0, 16), (2, 2)))
    expert_up = centred(seeds[11], (EXPERTS, D, FFE), D ** -0.5, 0.125, ((0, 16), (2, 2)))
    expert_down = centred(seeds[12], (EXPERTS, FFE, D), FFE ** -0.5, 0.1875, ((0, 16), (1, 2)))
    return dict(out_grad=out_grad, moe_input=moe_input, routes=routes, route_weights=route_weights, conv_result=conv_result, glu_value=glu_value, glu_gate=glu_gate, conv_taps=conv_taps, norm_gain=norm_gain, proj_weight=proj_weight, expert_gate=expert_gate, expert_up=expert_up, expert_down=expert_down)


norm_eps = 1e-05

def contract_rows(left, right):
    return lax.dot_general(left, right, (((0,), (0,)), ((), ())), preferred_element_type=jnp.float32)

def reference(out_grad, moe_input, routes, route_weights, conv_result, glu_value, glu_gate, conv_taps, norm_gain, proj_weight, expert_gate, expert_up, expert_down):
    slots = N_SP * CAP
    assigned = TOKENS * TOP
    flat = routes.reshape(N_SP, TOK_DEV * TOP).astype(jnp.int32)
    onehot = (flat[:, :, None] == jnp.arange(EXPERTS, dtype=jnp.int32)[None, None, :]).astype(jnp.int32)
    earlier = jnp.cumsum(onehot, axis=1) - onehot
    slot_index = lax.optimization_barrier(jnp.sum(earlier * onehot, axis=2))
    position = (jnp.arange(N_SP, dtype=jnp.int32)[:, None] * CAP + slot_index).reshape(-1).astype(jnp.int32)
    expert_flat = flat.reshape(-1)
    table = jnp.full((EXPERTS, slots), assigned, jnp.int32).at[expert_flat, position].set(jnp.arange(assigned, dtype=jnp.int32))
    grad_padded = jnp.concatenate([out_grad, jnp.zeros((1, D), jnp.bfloat16)], axis=0)
    input_padded = jnp.concatenate([moe_input, jnp.zeros((1, D), jnp.bfloat16)], axis=0)
    weight_padded = jnp.concatenate([route_weights.reshape(-1), jnp.zeros((1,), jnp.float32)])
    row_scale = float(slots) ** (-0.5)
    piece = FFE // N_TP

    def per_expert(args):
        index, weight_g, weight_u, weight_d = args
        token = jnp.where(index < assigned, index // TOP, TOKENS).astype(jnp.int32)
        inputs = input_padded[token]
        grads = (grad_padded[token].astype(jnp.float32) * weight_padded[index][:, None]).astype(jnp.bfloat16)
        gate_pre = jnp.dot(inputs, weight_g, preferred_element_type=jnp.float32)
        up_pre = jnp.dot(inputs, weight_u, preferred_element_type=jnp.float32)
        sigma = jax.nn.sigmoid(gate_pre)
        silu_gate = gate_pre * sigma
        hidden = (silu_gate * up_pre).astype(jnp.bfloat16)
        down_g = contract_rows(hidden, grads) * row_scale
        hidden_grad = lax.dot_general(grads, weight_d, (((1,), (1,)), ((), ())), preferred_element_type=jnp.float32)
        gate_back = (hidden_grad * up_pre * sigma * (1.0 + gate_pre * (1.0 - sigma))).astype(jnp.bfloat16)
        up_back = (hidden_grad * silu_gate).astype(jnp.bfloat16)
        gate_g = contract_rows(inputs, gate_back) * row_scale
        up_g = contract_rows(inputs, up_back) * row_scale
        back_gate = jnp.einsum('rpf,dpf->prd', gate_back.reshape(slots, N_TP, piece).astype(jnp.float32), weight_g.reshape(D, N_TP, piece).astype(jnp.float32))
        back_up = jnp.einsum('rpf,dpf->prd', up_back.reshape(slots, N_TP, piece).astype(jnp.float32), weight_u.reshape(D, N_TP, piece).astype(jnp.float32))
        partial_value = lax.optimization_barrier((back_gate + back_up).astype(jnp.bfloat16)).astype(jnp.float32)
        rows_back = lax.optimization_barrier(jnp.sum(partial_value, axis=0)).astype(jnp.bfloat16)
        return (gate_g, up_g, down_g, rows_back)
    gate_grad, up_grad, down_grad, returned = lax.map(per_expert, (table, expert_gate, expert_up, expert_down))
    contrib = returned.reshape(EXPERTS * slots, D)[(expert_flat * slots + position).astype(jnp.int32)]
    total = out_grad.astype(jnp.float32) + lax.optimization_barrier(jnp.sum(contrib.reshape(TOKENS, TOP, D).astype(jnp.float32), axis=1))
    input_grad = total.astype(jnp.bfloat16)
    values = conv_result.astype(jnp.float32)
    center = lax.optimization_barrier(jnp.mean(values, axis=1, keepdims=True))
    spread = lax.optimization_barrier(jnp.mean(values * values, axis=1, keepdims=True)) - center * center
    inv_std = lax.rsqrt(spread + norm_eps)
    normed = (values - center) * inv_std
    scaled = normed * norm_gain[None, :]
    sig_norm = jax.nn.sigmoid(scaled)
    activ = (scaled * sig_norm).astype(jnp.bfloat16)
    proj_grad = contract_rows(input_grad, activ) * float(TOKENS) ** (-0.5)
    act_grad = jnp.dot(input_grad, proj_weight, preferred_element_type=jnp.float32)
    norm_grad = act_grad * sig_norm * (1.0 + scaled * (1.0 - sig_norm)) * norm_gain[None, :]
    first = lax.optimization_barrier(jnp.mean(norm_grad, axis=1, keepdims=True))
    second = lax.optimization_barrier(jnp.mean(norm_grad * normed, axis=1, keepdims=True))
    conv_grad = inv_std * (norm_grad - first - normed * second)
    extended = jnp.concatenate([conv_grad, jnp.zeros((CONV_K - 1, CH), jnp.float32)], axis=0)
    taps_float = conv_taps.astype(jnp.float32)
    mixed_grad = jnp.zeros((TOKENS, CH), jnp.float32)
    for lag in range(CONV_K):
        mixed_grad = mixed_grad + taps_float[CONV_K - 1 - lag][None, :] * extended[lag:lag + TOKENS]
    sig_gate = jax.nn.sigmoid(glu_gate.astype(jnp.float32))
    value_grad = (mixed_grad * sig_gate).astype(jnp.bfloat16)
    gate_side_grad = (mixed_grad * glu_value.astype(jnp.float32) * sig_gate * (1.0 - sig_gate)).astype(jnp.bfloat16)
    return (input_grad, proj_grad, gate_grad, up_grad, down_grad, value_grad, gate_side_grad)
```

```python
import functools

import jax
import jax.numpy as jnp
from jax import lax
from jax.experimental import pallas as pl
from jax.experimental.pallas import tpu as pltpu
from jax.sharding import PartitionSpec as P

norm_eps = 1e-05
MESH = pl.DeviceIdType.MESH


def from_behind(shard, axis, by):
    count = lax.axis_size(axis)
    pairs = [(i, i + by) for i in range(count) if 0 <= i + by < count]
    return lax.ppermute(shard, axis, pairs)


def contract_rows(left, right):
    return lax.dot_general(
        left, right, (((0,), (0,)), ((), ())), preferred_element_type=jnp.float32
    )


def contract_cols(left, right):
    return lax.dot_general(
        left, right, (((1,), (1,)), ((), ())), preferred_element_type=jnp.float32
    )


def exchange_body(n, number, relay, lanes, *refs):
    xs, outs = refs[:number], refs[number : 2 * number]
    own_sem, send_sem, recv_sem = refs[2 * number : 2 * number + 3]
    fwd_send, fwd_recv = refs[2 * number + 3 :] if relay else (None, None)
    me = lax.axis_index("sp")
    half = lax.axis_index("tp")
    other = 1 - half

    def place(a, source, side):
        if not relay:
            return outs[a].at[source]
        if lanes:
            cols = xs[a].shape[2]
            return outs[a].at[source, :, pl.ds(pl.multiple_of(side * cols, cols), cols)]
        return outs[a].at[side, source]

    def outgoing(a, step):
        peer = lax.rem(me + step, n)
        return pltpu.make_async_remote_copy(
            src_ref=xs[a].at[peer],
            dst_ref=place(a, me, half),
            send_sem=send_sem.at[a, step],
            recv_sem=recv_sem.at[a, step],
            device_id=(peer, half),
            device_id_type=MESH,
        )

    def incoming(a, step):
        peer = lax.rem(me + step, n)
        source = lax.rem(me + n - step, n)
        return pltpu.make_async_remote_copy(
            src_ref=xs[a].at[peer],
            dst_ref=place(a, source, half),
            send_sem=send_sem.at[a, step],
            recv_sem=recv_sem.at[a, step],
            device_id=(peer, half),
            device_id_type=MESH,
        )

    def relayed(a, step, first=False):
        source = lax.rem(me + n - step, n)
        return pltpu.make_async_remote_copy(
            src_ref=xs[a].at[me] if first else place(a, source, half),
            dst_ref=place(a, source, half),
            send_sem=fwd_send.at[a, step],
            recv_sem=fwd_recv.at[a, step],
            device_id=(me, other),
            device_id_type=MESH,
        )

    def from_other(a, step):
        source = lax.rem(me + n - step, n)
        return pltpu.make_async_remote_copy(
            src_ref=xs[a].at[me],
            dst_ref=place(a, source, other),
            send_sem=fwd_send.at[a, step],
            recv_sem=fwd_recv.at[a, step],
            device_id=(me, other),
            device_id_type=MESH,
        )

    barrier = pltpu.get_barrier_semaphore()

    def greet(step, carry):
        pl.semaphore_signal(
            barrier, inc=1, device_id=(lax.rem(me + step, n), half), device_id_type=MESH
        )
        return carry

    lax.fori_loop(1, n, greet, 0)
    if relay:
        pl.semaphore_signal(barrier, inc=1, device_id=(me, other), device_id_type=MESH)
    pl.semaphore_wait(barrier, n - 1 + (1 if relay else 0))

    for a in range(number):

        def send(step, carry, a=a):
            outgoing(a, step).start()
            return carry

        lax.fori_loop(1, n, send, 0)
    own = []
    for a in range(number):
        own.append(pltpu.make_async_copy(xs[a].at[me], place(a, me, half), own_sem.at[a]))
        own[-1].start()
        if relay:
            relayed(a, 0, first=True).start()
    for a in range(number):

        def arrive(step, carry, a=a):
            incoming(a, step).wait_recv()
            if relay:
                relayed(a, step).start()
            return carry

        lax.fori_loop(1, n, arrive, 0)
    for a in range(number):

        def finish(step, carry, a=a):
            outgoing(a, step).wait_send()
            if relay:
                relayed(a, step).wait_send()
                from_other(a, step).wait_recv()
            return carry

        lax.fori_loop(1, n, finish, 0)
        own[a].wait()
        if relay:
            relayed(a, 0, first=True).wait_send()
            from_other(a, 0).wait_recv()


def exchange(arrays, collective_id, relay=True, lanes=True):
    n = lax.axis_size("sp")
    number = len(arrays)
    outs = []
    for x in arrays:
        shape = x.shape
        if relay:
            shape = (shape[0], shape[1], 2 * shape[2]) if lanes else (2,) + shape
        outs.append(jax.ShapeDtypeStruct(shape, x.dtype))
    sems = [pltpu.SemaphoreType.DMA((number,))] + [pltpu.SemaphoreType.DMA((number, n))] * (
        4 if relay else 2
    )
    return pl.pallas_call(
        functools.partial(exchange_body, n, number, relay, lanes),
        out_shape=tuple(outs),
        in_specs=[pl.BlockSpec(memory_space=pltpu.VMEM)] * number,
        out_specs=tuple([pl.BlockSpec(memory_space=pl.ANY)] * number),
        scratch_shapes=sems,
        compiler_params=pltpu.CompilerParams(collective_id=collective_id, has_side_effects=True),
    )(*arrays)


def per_device(
    out_grad,
    moe_input,
    routes,
    route_weights,
    conv_result,
    glu_value,
    glu_gate,
    conv_taps,
    norm_gain,
    proj_weight,
    expert_gate,
    expert_up,
    expert_down,
):
    n_sp = lax.axis_size("sp")
    n_tp = lax.axis_size("tp")
    half = lax.axis_index("tp")
    tok_rows, width = out_grad.shape
    top_count = routes.shape[1]
    capacity = 2 * top_count * tok_rows // n_sp
    slots = n_sp * capacity
    share = width // n_tp
    experts = jnp.arange(n_sp, dtype=jnp.int32)[None, :]
    named = [(routes[:, k : k + 1] == experts) for k in range(top_count)]
    per_token = sum(hit.astype(jnp.bfloat16) for hit in named)
    order = jnp.arange(tok_rows, dtype=jnp.int32)
    before = (order[None, :] < order[:, None]).astype(jnp.bfloat16)
    earlier = jnp.dot(before, per_token, preferred_element_type=jnp.float32).astype(jnp.int32)
    rows = jnp.arange(slots, dtype=jnp.int32)
    chosen = []
    for k in range(top_count):
        slot = jnp.sum(jnp.where(named[k], earlier, 0), axis=1)
        target = routes[:, k] * capacity + slot
        chosen.append(rows[:, None] == target[None, :])
    pick = functools.reduce(jnp.logical_or, chosen).astype(jnp.bfloat16)
    row_weight = sum(
        jnp.sum(jnp.where(chosen[k], route_weights[:, k][None, :], 0.0), axis=1)
        for k in range(top_count)
    )
    input_half = lax.dynamic_slice_in_dim(moe_input, half * share, share, 1)
    grad_half = lax.dynamic_slice_in_dim(out_grad, half * share, share, 1)
    send_input = jnp.dot(pick, input_half, preferred_element_type=jnp.float32).astype(jnp.bfloat16)
    send_grad = (
        jnp.dot(pick, grad_half, preferred_element_type=jnp.float32) * row_weight[:, None]
    ).astype(jnp.bfloat16)
    row_scale = float(slots) ** (-0.5)
    blocks = (n_sp, capacity, share)
    inputs, grads = exchange([send_input.reshape(blocks), send_grad.reshape(blocks)], 1)
    inputs, grads = inputs.reshape(slots, width), grads.reshape(slots, width)

    values = conv_result.astype(jnp.float32)
    channels = conv_result.shape[1] * n_tp
    sums, squares = lax.psum((jnp.sum(values, axis=1), jnp.sum(values * values, axis=1)), "tp")
    center = sums / channels
    spread = squares / channels - center * center
    inv_std = lax.rsqrt(spread + norm_eps)[:, None]
    normed = (values - center[:, None]) * inv_std
    scaled = normed * norm_gain[None, :]
    sig_norm = jax.nn.sigmoid(scaled)
    activ = (scaled * sig_norm).astype(jnp.bfloat16)
    all_activ = lax.all_gather(activ, "sp", axis=0, tiled=True)

    gate_pre = jnp.dot(inputs, expert_gate[0], preferred_element_type=jnp.float32)
    up_pre = jnp.dot(inputs, expert_up[0], preferred_element_type=jnp.float32)
    sigma = jax.nn.sigmoid(gate_pre)
    silu_gate = gate_pre * sigma
    hidden = (silu_gate * up_pre).astype(jnp.bfloat16)
    down_g = contract_rows(hidden, grads) * row_scale
    hidden_grad = contract_cols(grads, expert_down[0])
    gate_back = (hidden_grad * up_pre * sigma * (1.0 + gate_pre * (1.0 - sigma))).astype(
        jnp.bfloat16
    )
    up_back = (hidden_grad * silu_gate).astype(jnp.bfloat16)
    gate_g = contract_rows(inputs, gate_back) * row_scale
    up_g = contract_rows(inputs, up_back) * row_scale

    def partial_of(side):
        weight_g = lax.dynamic_slice_in_dim(expert_gate[0], side * share, share, 0)
        weight_u = lax.dynamic_slice_in_dim(expert_up[0], side * share, share, 0)
        return (contract_cols(gate_back, weight_g) + contract_cols(up_back, weight_u)).astype(
            jnp.bfloat16
        )

    arrived = lax.ppermute(
        partial_of(1 - half), "tp", [(i, n_tp - 1 - i) for i in range(n_tp)]
    )
    summed = (partial_of(half).astype(jnp.float32) + arrived.astype(jnp.float32)).astype(
        jnp.bfloat16
    )
    (returned,) = exchange([summed.reshape(blocks)], 2, relay=False)
    returned = returned.reshape(slots, share)
    grad_share = (grad_half.astype(jnp.float32) + contract_rows(pick, returned)).astype(
        jnp.bfloat16
    )
    input_grad = lax.all_gather(grad_share, "tp", axis=1, tiled=True)

    act_grad = jnp.dot(input_grad, proj_weight, preferred_element_type=jnp.float32)
    part = tok_rows // n_tp
    mine = lax.dynamic_slice_in_dim(input_grad, half * part, part, 0)
    mine = mine.reshape(part, n_sp, width // n_sp).transpose(1, 0, 2)
    (features,) = exchange([mine], 3, lanes=False)
    features = features.transpose(1, 0, 2, 3).reshape(n_sp * tok_rows, width // n_sp)
    token_scale = float(tok_rows * n_sp) ** (-0.5)
    proj_grad = contract_rows(features, all_activ) * token_scale

    norm_grad = act_grad * sig_norm * (1.0 + scaled * (1.0 - sig_norm)) * norm_gain[None, :]
    first, second = lax.psum(
        (jnp.sum(norm_grad, axis=1), jnp.sum(norm_grad * normed, axis=1)), "tp"
    )
    conv_grad = inv_std * (
        norm_grad - first[:, None] / channels - normed * (second[:, None] / channels)
    )
    reach = conv_taps.shape[0]
    rim = from_behind(conv_grad[: reach - 1].astype(jnp.bfloat16), "sp", -1).astype(jnp.float32)
    extended = jnp.concatenate([conv_grad, rim], axis=0)
    taps_float = conv_taps.astype(jnp.float32)
    mixed_grad = jnp.zeros_like(conv_grad)
    for lag in range(reach):
        mixed_grad = (
            mixed_grad + taps_float[reach - 1 - lag][None, :] * extended[lag : lag + tok_rows]
        )
    sig_gate = jax.nn.sigmoid(glu_gate.astype(jnp.float32))
    value_grad = (mixed_grad * sig_gate).astype(jnp.bfloat16)
    gate_side_grad = (
        mixed_grad * glu_value.astype(jnp.float32) * sig_gate * (1.0 - sig_gate)
    ).astype(jnp.bfloat16)
    return (
        input_grad,
        proj_grad,
        gate_g[None],
        up_g[None],
        down_g[None],
        value_grad,
        gate_side_grad,
    )


def solution(mesh):
    in_specs = (
        P("sp", None),
        P("sp", None),
        P("sp", None),
        P("sp", None),
        P("sp", "tp"),
        P("sp", "tp"),
        P("sp", "tp"),
        P(None, "tp"),
        P("tp"),
        P(None, "tp"),
        P("sp", None, "tp"),
        P("sp", None, "tp"),
        P("sp", "tp", None),
    )
    out_specs = (
        P("sp", None),
        P("sp", "tp"),
        P("sp", None, "tp"),
        P("sp", None, "tp"),
        P("sp", "tp", None),
        P("sp", "tp"),
        P("sp", "tp"),
    )
    return jax.shard_map(
        per_device, mesh=mesh, in_specs=in_specs, out_specs=out_specs, check_vma=False
    )
```
